32 devices in a mesh: sp: 8 (over z, y), dp: 4 (over x, core).
Axes of the slice: x: 2, y: 2, z: 4, core: 2. Of those that a mesh axis runs over, the one named last changes fastest.
Arguments:
- queries: bfloat16 [4096, 6144], P(('dp', 'sp')), may hold values from -360 to 360
- latent: bfloat16 [4096, 1024], P(('dp', 'sp')), may hold values from -6 to 6
- rope_key: bfloat16 [4096, 64], P(('dp', 'sp')), may hold values from -6 to 6
- latent_gain: float32 [1024], replicated, may hold values from 0.1 to 1.9
- kv_weight: bfloat16 [1024, 8192], P(None, 'dp'), may hold values from -0.1875 to 0.1875
- gate: bfloat16 [4096, 4096], P(('dp', 'sp')), may hold values from -6 to 6
- out_gain: float32 [4096], replicated, may hold values from 0.1 to 1.9
Outputs:
- attended: bfloat16 [4096, 4096], P(('dp', 'sp'))
The draws below stay inside these ranges and needn't reach their ends.
All inputs are finite; a program needn't handle non-finite values.
Results may differ from the reference program's by a relative error of at most 0.007.
Values may be sent and summed in bfloat16 or wider, within the bound.
A program may use at most 128 MiB of HBM per device.

```python
import jax
import jax.numpy as jnp
from jax import lax

HEADS = 32
NOPE = 128
ROPE = 64
VDIM = 128
KV_RANK = 1024
SEQ_LEN = 1024
TOKENS = 4096


def draw_queries(key, part):
    values = jax.random.normal(key, (TOKENS, HEADS * (NOPE + ROPE)), jnp.float32)
    values = jnp.clip(values, -6.0, 6.0)
    return values.astype(jnp.bfloat16)


def steps_of(stream_key, extent, shards, low, largest):
    loudness = 1.0
    for dim, blocks in shards:
        steps = jax.random.uniform(jax.random.fold_in(jax.random.fold_in(stream_key, 6), dim), (blocks,), jnp.float32, low / len(shards), largest / len(shards))
        loudness = loudness * jnp.repeat(jnp.exp(steps), extent[dim] // blocks).reshape((-1,) + (1,) * (len(extent) - 1 - dim))
    return loudness


def bell_draw(own_key, shape, spread, limit, pieces=(), held_as=jnp.bfloat16):
    loudness = steps_of(own_key, shape, pieces, -0.22, 0.18) if pieces else 1.0
    values = jax.random.normal(own_key, shape, jnp.float32) * spread * loudness
    return jnp.minimum(jnp.maximum(values, -limit), limit).astype(held_as)


def setup_inputs(seed: int = 0) -> dict:
    streams_of = jax.random.split(jax.random.key(seed), 8)
    return {
        "queries": draw_queries(jax.random.fold_in(streams_of[7], 71), 0),
        "latent": bell_draw(streams_of[1], (TOKENS, KV_RANK), 1.0, 6.0, ((0, 32),)),
        "rope_key": bell_draw(streams_of[2], (TOKENS, ROPE), 1.0, 6.0, ((0, 32),)),
        "latent_gain": jnp.clip(1.0 + 0.18 * jax.random.normal(streams_of[3], (KV_RANK,), jnp.float32), 0.1, 1.9),
        "kv_weight": bell_draw(streams_of[4], (KV_RANK, HEADS * (NOPE + VDIM)), KV_RANK ** -0.5, 0.1875, ((1, 4),)),
        "gate": bell_draw(streams_of[5], (TOKENS, HEADS * VDIM), 1.0, 6.0, ((0, 32),)),
        "out_gain": jnp.clip(1.0 + 0.18 * jax.random.normal(streams_of[6], (HEADS * VDIM,), jnp.float32), 0.1, 1.9),
    }


EPS = 1e-06
THETA = 10000.0

def rotary(values, position):
    half_width = values.shape[-1] // 2
    inverse = THETA ** (-jnp.arange(half_width, dtype=jnp.float32) / half_width)
    angles = position.astype(jnp.float32)[:, None] * inverse[None, :]
    if values.ndim == 3:
        angles = angles[:, None, :]
    cosine = jnp.cos(angles)
    sine_part = jnp.sin(angles)
    front_half = values[..., :half_width].astype(jnp.float32)
    back_half = values[..., half_width:].astype(jnp.float32)
    turned = jnp.concatenate([front_half * cosine - back_half * sine_part, back_half * cosine + front_half * sine_part], axis=-1)
    return turned.astype(jnp.bfloat16)

def attend(query_block, keys_plain, keys_rotated, values):
    scores = jnp.einsum('qhd,khd->hqk', query_block[..., :NOPE].astype(jnp.float32), keys_plain.astype(jnp.float32))
    scores = scores + jnp.einsum('qhr,kr->hqk', query_block[..., NOPE:].astype(jnp.float32), keys_rotated.astype(jnp.float32))
    scores = scores * (NOPE + ROPE) ** (-0.5)
    row_max = lax.optimization_barrier(jnp.max(scores, axis=-1, keepdims=True))
    raised = jnp.exp(scores - row_max)
    weights = (raised / lax.optimization_barrier(jnp.sum(raised, axis=-1, keepdims=True))).astype(jnp.bfloat16)
    result = jnp.einsum('hqk,khd->qhd', weights.astype(jnp.float32), values.astype(jnp.float32))
    return result.astype(jnp.bfloat16)

def reference(queries, latent, rope_key, latent_gain, kv_weight, gate, out_gain):
    rows_all = queries.shape[0]
    position = jnp.arange(rows_all, dtype=jnp.int32) % SEQ_LEN
    widened = latent.astype(jnp.float32)
    normed = (widened * lax.rsqrt(lax.optimization_barrier(jnp.mean(widened * widened, axis=-1, keepdims=True)) + EPS) * latent_gain.astype(jnp.float32)).astype(jnp.bfloat16)
    keyval = jnp.dot(normed, kv_weight, preferred_element_type=jnp.float32).astype(jnp.bfloat16)
    head_queries = queries.reshape(rows_all, HEADS, NOPE + ROPE)
    head_queries = jnp.concatenate([head_queries[..., :NOPE], rotary(head_queries[..., NOPE:], position)], axis=-1)
    keys_rotated = rotary(rope_key, position)
    seq_count = rows_all // SEQ_LEN
    block_rows = min(512, SEQ_LEN)
    block_count = SEQ_LEN // block_rows

    def one_sequence(operands):
        query_seq, kv_seq, rope_seq = operands
        keys_plain = kv_seq[..., :NOPE]
        values = kv_seq[..., NOPE:]
        blocks = query_seq.reshape(block_count, block_rows, HEADS, NOPE + ROPE)
        result = lax.map(lambda piece_rows: attend(piece_rows, keys_plain, rope_seq, values), blocks)
        return result.reshape(SEQ_LEN, HEADS * VDIM)
    heads_out = lax.map(one_sequence, (head_queries.reshape(seq_count, SEQ_LEN, HEADS, NOPE + ROPE), keyval.reshape(seq_count, SEQ_LEN, HEADS, NOPE + VDIM), keys_rotated.reshape(seq_count, SEQ_LEN, ROPE)))
    heads_out = heads_out.reshape(rows_all, HEADS * VDIM)
    gated_rows = heads_out.astype(jnp.float32) * jax.nn.silu(gate.astype(jnp.float32))
    scale_rows = lax.rsqrt(lax.optimization_barrier(jnp.mean(gated_rows * gated_rows, axis=-1, keepdims=True)) + EPS)
    return (gated_rows * scale_rows * out_gain.astype(jnp.float32)).astype(jnp.bfloat16)
```

```python
import functools

import jax
import jax.numpy as jnp
import numpy as np
from jax import lax
from jax.experimental import pallas as pl
from jax.experimental.pallas import tpu as pltpu
from jax.sharding import PartitionSpec as P

HEADS = 32
NOPE = 128
ROPE = 64
VDIM = 128
QDIM = NOPE + ROPE
KDIM = 256

EPS = 1e-06
THETA = 10000.0
LOG2E = 1.4426950408889634

MESH = pl.DeviceIdType.MESH
DN_T = (((1,), (1,)), ((), ()))


def turn(x, cosine, sine, mask):
    partner = jnp.where(mask, pltpu.roll(x, 96, 1), pltpu.roll(x, 32, 1))
    return x * cosine + partner * sine


def kernel(
    n_s, n_d,
    q_ref, lat_ref, rk_ref, lgain_ref, w_ref, gate_ref, ogain_ref, ta_ref, tb_ref,
    out_ref,
    w_v, gate_v, latb, rkb, qb, kbuf, vbuf, rq, ob, orecv,
    w_sem, gate_sem, lat_send, lat_recv, rk_send, rk_recv, relay_lat, relay_rk,
    q_send, q_recv, o_send, o_recv,
):
    s, d = lax.axis_index("sp"), lax.axis_index("dp")
    rows = lat_ref.shape[0]
    heads = HEADS // n_d
    qcols, ocols = heads * QDIM, heads * VDIM
    groups = n_s // n_d
    zh, m = s // n_d, s % n_d
    core = d % 2
    partner = d + 1 - 2 * core

    def send(src, dst, ssem, rsem, ts, td):
        same = (ts == s) & (td == d)

        @pl.when(jnp.logical_not(same))
        def _():
            pltpu.make_async_remote_copy(
                src, dst, ssem, rsem, device_id={"sp": ts, "dp": td}, device_id_type=MESH
            ).start()

        @pl.when(same)
        def _():
            pltpu.make_async_copy(src, dst, rsem).start()

    def sent(src, dst, ssem, rsem, ts, td):
        same = (ts == s) & (td == d)

        @pl.when(jnp.logical_not(same))
        def _():
            pltpu.make_async_remote_copy(
                src, dst, ssem, rsem, device_id={"sp": ts, "dp": td}, device_id_type=MESH
            ).wait_send()

    def arrived(dst, rsem):
        pltpu.make_async_copy(dst, dst, rsem).wait()

    latent_sends = []
    for k in range(groups):
        for pair in range(n_d // 2):
            i = k * (n_d // 2) + pair
            to = (k * n_d + d, 2 * pair + s % 2)
            latent_sends.append((lat_ref, latb.at[s], lat_send.at[i], lat_recv.at[s], *to))
            latent_sends.append((rk_ref, rkb.at[s], rk_send.at[i], rk_recv.at[s], *to))
    query_sends = [
        (
            q_ref.at[:, pl.ds(t * qcols, qcols)], qb.at[m], q_send.at[t], q_recv.at[m],
            zh * n_d + d, jnp.int32(t),
        )
        for t in range(n_d)
    ]
    w_copy = pltpu.make_async_copy(w_ref, w_v, w_sem)
    gate_copy = pltpu.make_async_copy(gate_ref, gate_v, gate_sem)

    for args in latent_sends + query_sends:
        send(*args)
    w_copy.start()
    gate_copy.start()
    w_copy.wait()

    lane = lax.broadcasted_iota(jnp.int32, (rows, 128), 1)
    low = lane < 64
    mask = (lane % 64) < 32
    sign = jnp.where(mask, -1.0, 1.0).astype(jnp.float32)

    def tables(block):
        ca, sa = ta_ref[0], ta_ref[1]
        cb, sb = tb_ref[0, block], tb_ref[1, block]
        return ca * cb - sa * sb, (sa * cb + ca * sb) * sign

    def key_step(i, carry):
        slot = lax.rem(s + i, n_s)
        at = pl.ds(pl.multiple_of(slot * rows, rows), rows)
        arrived(latb.at[slot], lat_recv.at[slot])
        arrived(rkb.at[slot], rk_recv.at[slot])

        @pl.when(slot % 2 == core)
        def _():
            for buf, ssem, rsem in ((latb, relay_lat, lat_recv), (rkb, relay_rk, rk_recv)):
                pltpu.make_async_remote_copy(
                    buf.at[slot], buf.at[slot], ssem.at[slot // 2], rsem.at[slot],
                    device_id={"sp": s, "dp": partner}, device_id_type=MESH,
                ).start()

        wide = latb[slot].astype(jnp.float32)
        scale = lax.rsqrt(jnp.mean(wide * wide, axis=-1, keepdims=True) + EPS)
        normed = (wide * scale * lgain_ref[...]).astype(jnp.bfloat16)
        cosine, sine = tables(slot)
        raw = rkb[slot].astype(jnp.float32)
        rot = turn(jnp.concatenate([raw, jnp.zeros_like(raw)], axis=1), cosine, sine, mask)
        rot_high = pltpu.roll(rot, 64, 1)
        for h in range(heads):
            both = jnp.dot(
                normed, w_v[:, h * 256 : (h + 1) * 256], preferred_element_type=jnp.float32
            )
            plain = both[:, :NOPE]
            if h % 2 == 0:
                first, second = plain, rot
            else:
                moved = pltpu.roll(plain, 64, 1)
                first = jnp.where(low, 0.0, moved)
                second = jnp.where(low, moved, rot_high)
            kbuf[h, at, :128] = first.astype(jnp.bfloat16)
            kbuf[h, at, 128:] = second.astype(jnp.bfloat16)
            vbuf[h, at, :VDIM] = both[:, NOPE:].astype(jnp.bfloat16)
            vbuf[h, at, VDIM:] = jnp.ones((rows, 128), jnp.bfloat16)
        return carry

    lax.fori_loop(0, n_s, key_step, 0)

    factor = LOG2E * QDIM ** -0.5

    def output_send(j):
        return (ob.at[j], orecv.at[d], o_send.at[j], o_recv.at[d], zh * n_d + j, m)

    def query_step(r, carry):
        for half in range(2):
            slot = 2 * r + half
            arrived(qb.at[slot], q_recv.at[slot])
            cosine, sine = tables(zh * n_d + slot)
            cosine_high, sine_high = pltpu.roll(cosine, 64, 1), pltpu.roll(sine, 64, 1)
            here = slice(half * rows, (half + 1) * rows)
            for p in range(heads // 2):
                c = p * 2 * QDIM
                rq[here, c : c + 128] = qb[slot, :, c : c + 128]
                x = qb[slot, :, c + 128 : c + 256].astype(jnp.float32)
                rq[here, c + 128 : c + 256] = turn(x, cosine, sine, mask).astype(jnp.bfloat16)
                x = qb[slot, :, c + 256 : c + 384].astype(jnp.float32)
                rq[here, c + 256 : c + 384] = turn(x, cosine_high, sine_high, mask).astype(jnp.bfloat16)

        def head_pair(p, carry):
            for odd in range(2):
                h = 2 * p + odd
                col = pl.multiple_of(p * (2 * QDIM) + odd * 128, 128)
                scores = lax.dot_general(
                    rq[:, pl.ds(col, KDIM)], kbuf[h], DN_T, preferred_element_type=jnp.float32
                )
                top = jnp.max(scores, axis=-1, keepdims=True)
                raised = jnp.exp2((scores - top) * factor).astype(jnp.bfloat16)
                total = jnp.dot(raised, vbuf[h], preferred_element_type=jnp.float32)
                result = (total[:, :VDIM] / total[:, VDIM:]).astype(jnp.bfloat16)
                at = pl.ds(pl.multiple_of(h * VDIM, VDIM), VDIM)
                ob[2 * r, :, at] = result[:rows]
                ob[2 * r + 1, :, at] = result[rows:]
            return carry

        lax.fori_loop(0, heads // 2, head_pair, 0)
        send(*output_send(2 * r))
        send(*output_send(2 * r + 1))
        return carry

    lax.fori_loop(0, n_d // 2, query_step, 0)

    gate_copy.wait()
    square = jnp.zeros((rows, 1), jnp.float32)
    for t in range(n_d):
        arrived(orecv.at[t], o_recv.at[t])
        g = gate_v[:, t * ocols : (t + 1) * ocols].astype(jnp.float32)
        gated = orecv[t].astype(jnp.float32) * (g / (1.0 + jnp.exp(-g)))
        square = square + jnp.sum(gated * gated, axis=-1, keepdims=True)
    scale = lax.rsqrt(square / (HEADS * VDIM) + EPS)
    for t in range(n_d):
        cols = slice(t * ocols, (t + 1) * ocols)
        g = gate_v[:, cols].astype(jnp.float32)
        gated = orecv[t].astype(jnp.float32) * (g / (1.0 + jnp.exp(-g)))
        out_ref[:, cols] = (gated * scale * ogain_ref[:, cols]).astype(jnp.bfloat16)

    for args in latent_sends + query_sends:
        sent(*args)
    for half in range(n_s // 2):
        slot = 2 * half + core
        for buf, ssem, rsem in ((latb, relay_lat, lat_recv), (rkb, relay_rk, rk_recv)):
            pltpu.make_async_remote_copy(
                buf.at[slot], buf.at[slot], ssem.at[half], rsem.at[slot],
                device_id={"sp": s, "dp": partner}, device_id_type=MESH,
            ).wait_send()
    for j in range(n_d):
        sent(*output_send(j))


def angle_tables(rows, n_s):
    half = ROPE // 2
    inverse = np.zeros(128)
    inverse[:ROPE] = np.tile(THETA ** (-np.arange(half) / half), 2)
    inner = np.arange(rows)[:, None] * inverse[None, :]
    outer = (np.arange(n_s) * rows)[:, None] * inverse[None, :]
    inner = np.stack([np.cos(inner), np.sin(inner)]).astype(np.float32)
    outer = np.stack([np.cos(outer), np.sin(outer)]).astype(np.float32)
    return jnp.asarray(inner), jnp.asarray(outer[:, :, None, :])


def per_device(n_s, n_d, queries, latent, rope_key, latent_gain, kv_weight, gate, out_gain):
    rows, rank = latent.shape
    heads = HEADS // n_d
    seq = rows * n_s
    inner, outer = angle_tables(rows, n_s)
    bf = jnp.bfloat16
    dma = pltpu.SemaphoreType.DMA
    vmem = pl.BlockSpec(memory_space=pltpu.VMEM)
    hbm = pl.BlockSpec(memory_space=pl.ANY)
    pieces = n_s // 2
    return pl.pallas_call(
        functools.partial(kernel, n_s, n_d),
        out_shape=jax.ShapeDtypeStruct(gate.shape, bf),
        in_specs=[hbm, vmem, vmem, vmem, hbm, hbm, vmem, vmem, vmem],
        out_specs=vmem,
        scratch_shapes=[
            pltpu.VMEM(kv_weight.shape, bf),
            pltpu.VMEM(gate.shape, bf),
            pltpu.VMEM((n_s, rows, rank), bf),
            pltpu.VMEM((n_s, rows, ROPE), bf),
            pltpu.VMEM((n_d, rows, heads * QDIM), bf),
            pltpu.VMEM((heads, seq, KDIM), bf),
            pltpu.VMEM((heads, seq, 2 * VDIM), bf),
            pltpu.VMEM((2 * rows, heads * QDIM), bf),
            pltpu.VMEM((n_d, rows, heads * VDIM), bf),
            pltpu.VMEM((n_d, rows, heads * VDIM), bf),
            dma, dma,
            dma((pieces,)), dma((n_s,)), dma((pieces,)), dma((n_s,)),
            dma((pieces,)), dma((pieces,)),
            dma((n_d,)), dma((n_d,)), dma((n_d,)), dma((n_d,)),
        ],
        compiler_params=pltpu.CompilerParams(
            has_side_effects=True, vmem_limit_bytes=60 * 1024 * 1024
        ),
        name="latent_attention",
    )(
        queries, latent, rope_key, latent_gain[None, :], kv_weight, gate, out_gain[None, :],
        inner, outer,
    )


def solution(mesh):
    return jax.shard_map(
        functools.partial(per_device, mesh.shape["sp"], mesh.shape["dp"]),
        mesh=mesh,
        in_specs=(
            P(("dp", "sp"), None),
            P(("dp", "sp"), None),
            P(("dp", "sp"), None),
            P(),
            P(None, "dp"),
            P(("dp", "sp"), None),
            P(),
        ),
        out_specs=P(("dp", "sp"), None),
        check_vma=False,
    )
```

```python
import functools

import jax
import jax.numpy as jnp
import numpy as np
from jax import lax
from jax.experimental import pallas as pl
from jax.experimental.pallas import tpu as pltpu
from jax.sharding import PartitionSpec as P

HEADS = 32
NOPE = 128
ROPE = 64
VDIM = 128
QDIM = NOPE + ROPE
KDIM = 256

EPS = 1e-06
THETA = 10000.0
LOG2E = 1.4426950408889634

MESH = pl.DeviceIdType.MESH
DN_T = (((1,), (1,)), ((), ()))


def turn(x, cosine, sine, mask):
    partner = jnp.where(mask, pltpu.roll(x, 96, 1), pltpu.roll(x, 32, 1))
    return x * cosine + partner * sine


def kernel(
    n_s, n_d,
    q_ref, lat_ref, rk_ref, lgain_ref, w_ref, gate_ref, ogain_ref, ta_ref, tb_ref,
    out_ref,
    w_v, gate_v, latb, rkb, qb, kbuf, vbuf, rq, ob, orecv,
    w_sem, gate_sem, lat_send, lat_recv, rk_send, rk_recv, relay_lat, relay_rk,
    q_send, q_recv, o_send, o_recv,
):
    s, d = lax.axis_index("sp"), lax.axis_index("dp")
    rows = lat_ref.shape[0]
    heads = HEADS // n_d
    qcols, ocols = heads * QDIM, heads * VDIM
    groups = n_s // n_d
    half = n_d // 2
    zh, m = s // n_d, s % n_d
    seq = 2 * ((m % half - m // half + half) % half) + m // half
    home = (d % 2) * half + (d // 2 + d % 2) % half
    core = d % 2
    partner = d + 1 - 2 * core

    def send(src, dst, ssem, rsem, ts, td):
        same = (ts == s) & (td == d)

        @pl.when(jnp.logical_not(same))
        def _():
            pltpu.make_async_remote_copy(
                src, dst, ssem, rsem, device_id={"sp": ts, "dp": td}, device_id_type=MESH
            ).start()

        @pl.when(same)
        def _():
            pltpu.make_async_copy(src, dst, rsem).start()

    def sent(src, dst, ssem, rsem, ts, td):
        same = (ts == s) & (td == d)

        @pl.when(jnp.logical_not(same))
        def _():
            pltpu.make_async_remote_copy(
                src, dst, ssem, rsem, device_id={"sp": ts, "dp": td}, device_id_type=MESH
            ).wait_send()

    def arrived(dst, rsem):
        pltpu.make_async_copy(dst, dst, rsem).wait()

    latent_sends = []
    for k in range(groups):
        for pair in range(n_d // 2):
            i = k * (n_d // 2) + pair
            to = (k * n_d + home, 2 * pair + s % 2)
            latent_sends.append((lat_ref, latb.at[s], lat_send.at[i], lat_recv.at[s], *to))
            latent_sends.append((rk_ref, rkb.at[s], rk_send.at[i], rk_recv.at[s], *to))
    query_sends = [
        (
            q_ref.at[:, pl.ds(t * qcols, qcols)], qb.at[m], q_send.at[t], q_recv.at[m],
            zh * n_d + home, jnp.int32(t),
        )
        for t in range(n_d)
    ]
    w_copy = pltpu.make_async_copy(w_ref, w_v, w_sem)
    gate_copy = pltpu.make_async_copy(gate_ref, gate_v, gate_sem)

    for args in latent_sends + query_sends:
        send(*args)
    w_copy.start()
    gate_copy.start()
    w_copy.wait()

    lane = lax.broadcasted_iota(jnp.int32, (rows, 128), 1)
    low = lane < 64
    mask = (lane % 64) < 32
    sign = jnp.where(mask, -1.0, 1.0).astype(jnp.float32)

    def tables(block):
        ca, sa = ta_ref[0], ta_ref[1]
        cb, sb = tb_ref[0, block], tb_ref[1, block]
        return ca * cb - sa * sb, (sa * cb + ca * sb) * sign

    def nearest(i):
        if n_s & (n_s - 1):
            return (s + i) % n_s
        out, bit = 0, 1
        while bit < n_s:
            out = out + bit * ((s // bit + i // bit) % 2)
            bit *= 2
        return out

    def key_step(i, carry):
        slot = nearest(i)
        at = pl.ds(pl.multiple_of(slot * rows, rows), rows)
        arrived(latb.at[slot], lat_recv.at[slot])
        arrived(rkb.at[slot], rk_recv.at[slot])

        @pl.when(slot % 2 == core)
        def _():
            for buf, ssem, rsem in ((latb, relay_lat, lat_recv), (rkb, relay_rk, rk_recv)):
                pltpu.make_async_remote_copy(
                    buf.at[slot], buf.at[slot], ssem.at[slot // 2], rsem.at[slot],
                    device_id={"sp": s, "dp": partner}, device_id_type=MESH,
                ).start()

        wide = latb[slot].astype(jnp.float32)
        scale = lax.rsqrt(jnp.mean(wide * wide, axis=-1, keepdims=True) + EPS)
        normed = (wide * scale * lgain_ref[...]).astype(jnp.bfloat16)
        cosine, sine = tables(slot)
        raw = rkb[slot].astype(jnp.float32)
        rot = turn(jnp.concatenate([raw, jnp.zeros_like(raw)], axis=1), cosine, sine, mask)
        rot_high = pltpu.roll(rot, 64, 1)
        for h in range(heads):
            both = jnp.dot(
                normed, w_v[:, h * 256 : (h + 1) * 256], preferred_element_type=jnp.float32
            )
            plain = both[:, :NOPE]
            if h % 2 == 0:
                first, second = plain, rot
            else:
                moved = pltpu.roll(plain, 64, 1)
                first = jnp.where(low, 0.0, moved)
                second = jnp.where(low, moved, rot_high)
            kbuf[h, at, :128] = first.astype(jnp.bfloat16)
            kbuf[h, at, 128:] = second.astype(jnp.bfloat16)
            vbuf[h, at, :VDIM] = both[:, NOPE:].astype(jnp.bfloat16)
            vbuf[h, at, VDIM:] = jnp.ones((rows, 128), jnp.bfloat16)
        return carry

    lax.fori_loop(0, n_s, key_step, 0)

    factor = LOG2E * QDIM ** -0.5

    def output_send(j):
        return (ob.at[j], orecv.at[d], o_send.at[j], o_recv.at[d], zh * n_d + j, seq)

    def query_step(i, carry):
        r = (i + m // 2) % half
        for part in range(2):
            slot = 2 * r + part
            arrived(qb.at[slot], q_recv.at[slot])
            cosine, sine = tables(zh * n_d + slot)
            cosine_high, sine_high = pltpu.roll(cosine, 64, 1), pltpu.roll(sine, 64, 1)
            here = slice(part * rows, (part + 1) * rows)
            for p in range(heads // 2):
                c = p * 2 * QDIM
                rq[here, c : c + 128] = qb[slot, :, c : c + 128]
                x = qb[slot, :, c + 128 : c + 256].astype(jnp.float32)
                rq[here, c + 128 : c + 256] = turn(x, cosine, sine, mask).astype(jnp.bfloat16)
                x = qb[slot, :, c + 256 : c + 384].astype(jnp.float32)
                rq[here, c + 256 : c + 384] = turn(x, cosine_high, sine_high, mask).astype(jnp.bfloat16)

        def head_pair(p, carry):
            for odd in range(2):
                h = 2 * p + odd
                col = pl.multiple_of(p * (2 * QDIM) + odd * 128, 128)
                scores = lax.dot_general(
                    rq[:, pl.ds(col, KDIM)], kbuf[h], DN_T, preferred_element_type=jnp.float32
                )
                top = jnp.max(scores, axis=-1, keepdims=True)
                raised = jnp.exp2((scores - top) * factor).astype(jnp.bfloat16)
                total = jnp.dot(raised, vbuf[h], preferred_element_type=jnp.float32)
                result = (total[:, :VDIM] / total[:, VDIM:]).astype(jnp.bfloat16)
                at = pl.ds(pl.multiple_of(h * VDIM, VDIM), VDIM)
                ob[2 * r, :, at] = result[:rows]
                ob[2 * r + 1, :, at] = result[rows:]
            return carry

        lax.fori_loop(0, heads // 2, head_pair, 0)
        send(*output_send(2 * r))
        send(*output_send(2 * r + 1))
        return carry

    lax.fori_loop(0, half, query_step, 0)

    gate_copy.wait()
    square = jnp.zeros((rows, 1), jnp.float32)
    for t in range(n_d):
        arrived(orecv.at[t], o_recv.at[t])
        g = gate_v[:, t * ocols : (t + 1) * ocols].astype(jnp.float32)
        gated = orecv[t].astype(jnp.float32) * (g / (1.0 + jnp.exp(-g)))
        square = square + jnp.sum(gated * gated, axis=-1, keepdims=True)
    scale = lax.rsqrt(square / (HEADS * VDIM) + EPS)
    for t in range(n_d):
        cols = slice(t * ocols, (t + 1) * ocols)
        g = gate_v[:, cols].astype(jnp.float32)
        gated = orecv[t].astype(jnp.float32) * (g / (1.0 + jnp.exp(-g)))
        out_ref[:, cols] = (gated * scale * ogain_ref[:, cols]).astype(jnp.bfloat16)

    for args in latent_sends + query_sends:
        sent(*args)
    for part in range(n_s // 2):
        slot = 2 * part + core
        for buf, ssem, rsem in ((latb, relay_lat, lat_recv), (rkb, relay_rk, rk_recv)):
            pltpu.make_async_remote_copy(
                buf.at[slot], buf.at[slot], ssem.at[part], rsem.at[slot],
                device_id={"sp": s, "dp": partner}, device_id_type=MESH,
            ).wait_send()
    for j in range(n_d):
        sent(*output_send(j))


def angle_tables(rows, n_s):
    half = ROPE // 2
    inverse = np.zeros(128)
    inverse[:ROPE] = np.tile(THETA ** (-np.arange(half) / half), 2)
    inner = np.arange(rows)[:, None] * inverse[None, :]
    outer = (np.arange(n_s) * rows)[:, None] * inverse[None, :]
    inner = np.stack([np.cos(inner), np.sin(inner)]).astype(np.float32)
    outer = np.stack([np.cos(outer), np.sin(outer)]).astype(np.float32)
    return jnp.asarray(inner), jnp.asarray(outer[:, :, None, :])


def per_device(n_s, n_d, queries, latent, rope_key, latent_gain, kv_weight, gate, out_gain):
    rows, rank = latent.shape
    heads = HEADS // n_d
    seq = rows * n_s
    inner, outer = angle_tables(rows, n_s)
    bf = jnp.bfloat16
    dma = pltpu.SemaphoreType.DMA
    vmem = pl.BlockSpec(memory_space=pltpu.VMEM)
    hbm = pl.BlockSpec(memory_space=pl.ANY)
    pieces = n_s // 2
    return pl.pallas_call(
        functools.partial(kernel, n_s, n_d),
        out_shape=jax.ShapeDtypeStruct(gate.shape, bf),
        in_specs=[hbm, vmem, vmem, vmem, hbm, hbm, vmem, vmem, vmem],
        out_specs=vmem,
        scratch_shapes=[
            pltpu.VMEM(kv_weight.shape, bf),
            pltpu.VMEM(gate.shape, bf),
            pltpu.VMEM((n_s, rows, rank), bf),
            pltpu.VMEM((n_s, rows, ROPE), bf),
            pltpu.VMEM((n_d, rows, heads * QDIM), bf),
            pltpu.VMEM((heads, seq, KDIM), bf),
            pltpu.VMEM((heads, seq, 2 * VDIM), bf),
            pltpu.VMEM((2 * rows, heads * QDIM), bf),
            pltpu.VMEM((n_d, rows, heads * VDIM), bf),
            pltpu.VMEM((n_d, rows, heads * VDIM), bf),
            dma, dma,
            dma((pieces,)), dma((n_s,)), dma((pieces,)), dma((n_s,)),
            dma((pieces,)), dma((pieces,)),
            dma((n_d,)), dma((n_d,)), dma((n_d,)), dma((n_d,)),
        ],
        compiler_params=pltpu.CompilerParams(
            has_side_effects=True, vmem_limit_bytes=60 * 1024 * 1024
        ),
        name="latent_attention",
    )(
        queries, latent, rope_key, latent_gain[None, :], kv_weight, gate, out_gain[None, :],
        inner, outer,
    )


def solution(mesh):
    return jax.shard_map(
        functools.partial(per_device, mesh.shape["sp"], mesh.shape["dp"]),
        mesh=mesh,
        in_specs=(
            P(("dp", "sp"), None),
            P(("dp", "sp"), None),
            P(("dp", "sp"), None),
            P(),
            P(None, "dp"),
            P(("dp", "sp"), None),
            P(),
        ),
        out_specs=P(("dp", "sp"), None),
        check_vma=False,
    )
```

```python
import functools

import jax
import jax.numpy as jnp
import numpy as np
from jax import lax
from jax.experimental import pallas as pl
from jax.experimental.pallas import tpu as pltpu
from jax.sharding import PartitionSpec as P

HEADS = 32
NOPE = 128
ROPE = 64
VDIM = 128
QDIM = NOPE + ROPE
PAIR = 2 * QDIM
KDIM = 256

EPS = 1e-06
THETA = 10000.0
LOG2E = 1.4426950408889634

MESH = pl.DeviceIdType.MESH
DN_T = (((1,), (1,)), ((), ()))


def turn(x, cosine, sine, mask):
    partner = jnp.where(mask, pltpu.roll(x, 96, 1), pltpu.roll(x, 32, 1))
    return x * cosine + partner * sine


def kernel(
    n_s, n_d,
    q_ref, lat_ref, rk_ref, lgain_ref, w_ref, gate_ref, ogain_ref, ta_ref, tb_ref,
    out_ref,
    w_v, gate_v, latb, rkb, qb, kbuf, vbuf, rq, ob, orecv,
    w_sem, gate_sem, lat_send, lat_recv, rk_send, rk_recv, relay_lat, relay_rk,
    q_send, q_recv, o_send, o_recv,
):
    s, d = lax.axis_index("sp"), lax.axis_index("dp")
    rows = lat_ref.shape[0]
    heads = HEADS // n_d
    pairs = heads // 2
    groups = n_s // n_d
    half = n_d // 2
    zh, m = s // n_d, s % n_d
    seq = 2 * ((m % half - m // half + half) % half) + m // half
    home = (d % 2) * half + (d // 2 + d % 2) % half
    core = d % 2
    partner = d + 1 - 2 * core

    def send(src, dst, ssem, rsem, ts, td):
        same = (ts == s) & (td == d)

        @pl.when(jnp.logical_not(same))
        def _():
            pltpu.make_async_remote_copy(
                src, dst, ssem, rsem, device_id={"sp": ts, "dp": td}, device_id_type=MESH
            ).start()

        @pl.when(same)
        def _():
            pltpu.make_async_copy(src, dst, rsem).start()

    def sent(src, dst, ssem, rsem, ts, td):
        same = (ts == s) & (td == d)

        @pl.when(jnp.logical_not(same))
        def _():
            pltpu.make_async_remote_copy(
                src, dst, ssem, rsem, device_id={"sp": ts, "dp": td}, device_id_type=MESH
            ).wait_send()

    def arrived(dst, rsem):
        pltpu.make_async_copy(dst, dst, rsem).wait()

    latent_sends = []
    for k in range(groups):
        for pair in range(n_d // 2):
            i = k * (n_d // 2) + pair
            to = (k * n_d + home, 2 * pair + s % 2)
            latent_sends.append((lat_ref, latb.at[s], lat_send.at[i], lat_recv.at[s], *to))
            latent_sends.append((rk_ref, rkb.at[s], rk_send.at[i], rk_recv.at[s], *to))
    query_sends = [
        (
            q_ref.at[:, pl.ds((t * pairs + p) * PAIR, PAIR)], qb.at[m, p],
            q_send.at[t, p], q_recv.at[m, p], zh * n_d + home, jnp.int32(t),
        )
        for p in range(pairs)
        for t in range(n_d)
    ]
    w_copy = pltpu.make_async_copy(w_ref, w_v, w_sem)
    gate_copy = pltpu.make_async_copy(gate_ref, gate_v, gate_sem)

    for args in latent_sends + query_sends:
        send(*args)
    w_copy.start()
    gate_copy.start()
    w_copy.wait()

    lane = lax.broadcasted_iota(jnp.int32, (rows, 128), 1)
    low = lane < 64
    mask = (lane % 64) < 32
    sign = jnp.where(mask, -1.0, 1.0).astype(jnp.float32)

    def tables(block):
        ca, sa = ta_ref[0], ta_ref[1]
        cb, sb = tb_ref[0, block], tb_ref[1, block]
        return ca * cb - sa * sb, (sa * cb + ca * sb) * sign

    def nearest(i):
        if n_s & (n_s - 1):
            return (s + i) % n_s
        out, bit = 0, 1
        while bit < n_s:
            out = out + bit * ((s // bit + i // bit) % 2)
            bit *= 2
        return out

    def key_step(i, carry):
        slot = nearest(i)
        at = pl.ds(pl.multiple_of(slot * rows, rows), rows)
        arrived(latb.at[slot], lat_recv.at[slot])
        arrived(rkb.at[slot], rk_recv.at[slot])

        @pl.when(slot % 2 == core)
        def _():
            for buf, ssem, rsem in ((latb, relay_lat, lat_recv), (rkb, relay_rk, rk_recv)):
                pltpu.make_async_remote_copy(
                    buf.at[slot], buf.at[slot], ssem.at[slot // 2], rsem.at[slot],
                    device_id={"sp": s, "dp": partner}, device_id_type=MESH,
                ).start()

        wide = latb[slot].astype(jnp.float32)
        scale = lax.rsqrt(jnp.mean(wide * wide, axis=-1, keepdims=True) + EPS)
        normed = (wide * scale * lgain_ref[...]).astype(jnp.bfloat16)
        cosine, sine = tables(slot)
        raw = rkb[slot].astype(jnp.float32).T
        rot = turn(jnp.concatenate([raw, jnp.zeros_like(raw)], axis=1), cosine, sine, mask)
        rot_high = pltpu.roll(rot, 64, 1)
        for h in range(heads):
            both = jnp.dot(
                normed, w_v[:, h * 256 : (h + 1) * 256], preferred_element_type=jnp.float32
            )
            plain = both[:, :NOPE]
            if h % 2 == 0:
                first, second = plain, rot
            else:
                moved = pltpu.roll(plain, 64, 1)
                first = jnp.where(low, 0.0, moved)
                second = jnp.where(low, moved, rot_high)
            kbuf[h, at, :128] = first.astype(jnp.bfloat16)
            kbuf[h, at, 128:] = second.astype(jnp.bfloat16)
            vbuf[h, at, :VDIM] = both[:, NOPE:].astype(jnp.bfloat16)
            vbuf[h, at, VDIM:] = jnp.ones((rows, 128), jnp.bfloat16)
        return carry

    lax.fori_loop(0, n_s, key_step, 0)

    factor = LOG2E * QDIM ** -0.5

    def output_send(j, p):
        return (ob.at[j, p], orecv.at[d, p], o_send.at[j, p], o_recv.at[d, p], zh * n_d + j, seq)

    def query_step(i, carry):
        r, p = (i // pairs + m // 2) % half, i % pairs
        for part in range(2):
            slot = 2 * r + part
            arrived(qb.at[slot, p], q_recv.at[slot, p])
            cosine, sine = tables(zh * n_d + slot)
            cosine_high, sine_high = pltpu.roll(cosine, 64, 1), pltpu.roll(sine, 64, 1)
            here = slice(part * rows, (part + 1) * rows)
            rq[here, :128] = qb[slot, p, :, :128]
            x = qb[slot, p, :, 128:256].astype(jnp.float32)
            rq[here, 128:256] = turn(x, cosine, sine, mask).astype(jnp.bfloat16)
            x = qb[slot, p, :, 256:].astype(jnp.float32)
            rq[here, 256:] = turn(x, cosine_high, sine_high, mask).astype(jnp.bfloat16)
        for odd in range(2):
            h = 2 * p + odd
            scores = lax.dot_general(
                rq[:, odd * 128 : odd * 128 + KDIM], kbuf[h], DN_T, preferred_element_type=jnp.float32
            )
            top = jnp.max(scores, axis=-1, keepdims=True)
            raised = jnp.exp2((scores - top) * factor).astype(jnp.bfloat16)
            total = jnp.dot(raised, vbuf[h], preferred_element_type=jnp.float32)
            result = (total[:, :VDIM] / total[:, VDIM:]).astype(jnp.bfloat16)
            at = slice(odd * VDIM, (odd + 1) * VDIM)
            ob[2 * r, p, :, at] = result[:rows]
            ob[2 * r + 1, p, :, at] = result[rows:]
        send(*output_send(2 * r, p))
        send(*output_send(2 * r + 1, p))
        return carry

    lax.fori_loop(0, half * pairs, query_step, 0)

    gate_copy.wait()
    def gated_piece(t, p):
        c = (t * pairs + p) * 2 * VDIM
        g = gate_v[:, c : c + 2 * VDIM].astype(jnp.float32)
        return slice(c, c + 2 * VDIM), orecv[t, p].astype(jnp.float32) * (g / (1.0 + jnp.exp(-g)))

    square = jnp.zeros((rows, 1), jnp.float32)
    for p in range(pairs):
        for t in range(n_d):
            arrived(orecv.at[t, p], o_recv.at[t, p])
            _, gated = gated_piece(t, p)
            square = square + jnp.sum(gated * gated, axis=-1, keepdims=True)
    scale = lax.rsqrt(square / (HEADS * VDIM) + EPS)
    for t in range(n_d):
        for p in range(pairs):
            cols, gated = gated_piece(t, p)
            out_ref[:, cols] = (gated * scale * ogain_ref[:, cols]).astype(jnp.bfloat16)

    for args in latent_sends + query_sends:
        sent(*args)
    for part in range(n_s // 2):
        slot = 2 * part + core
        for buf, ssem, rsem in ((latb, relay_lat, lat_recv), (rkb, relay_rk, rk_recv)):
            pltpu.make_async_remote_copy(
                buf.at[slot], buf.at[slot], ssem.at[part], rsem.at[slot],
                device_id={"sp": s, "dp": partner}, device_id_type=MESH,
            ).wait_send()

    def output_sent(i, carry):
        sent(*output_send(i // pairs, i % pairs))
        return carry

    lax.fori_loop(0, n_d * pairs, output_sent, 0)


def angle_tables(rows, n_s):
    half = ROPE // 2
    inverse = np.zeros(128)
    inverse[:ROPE] = np.tile(THETA ** (-np.arange(half) / half), 2)
    inner = np.arange(rows)[:, None] * inverse[None, :]
    outer = (np.arange(n_s) * rows)[:, None] * inverse[None, :]
    inner = np.stack([np.cos(inner), np.sin(inner)]).astype(np.float32)
    outer = np.stack([np.cos(outer), np.sin(outer)]).astype(np.float32)
    return jnp.asarray(inner), jnp.asarray(outer[:, :, None, :])


def per_device(n_s, n_d, queries, latent, rope_key, latent_gain, kv_weight, gate, out_gain):
    rows, rank = latent.shape
    heads = HEADS // n_d
    pairs = heads // 2
    seq = rows * n_s
    inner, outer = angle_tables(rows, n_s)
    bf = jnp.bfloat16
    dma = pltpu.SemaphoreType.DMA
    vmem = pl.BlockSpec(memory_space=pltpu.VMEM)
    hbm = pl.BlockSpec(memory_space=pl.ANY)
    pieces = n_s // 2
    return pl.pallas_call(
        functools.partial(kernel, n_s, n_d),
        out_shape=jax.ShapeDtypeStruct(gate.shape, bf),
        in_specs=[hbm, vmem, vmem, vmem, hbm, hbm, vmem, vmem, vmem],
        out_specs=vmem,
        scratch_shapes=[
            pltpu.VMEM(kv_weight.shape, bf),
            pltpu.VMEM(gate.shape, bf),
            pltpu.VMEM((n_s, rows, rank), bf),
            pltpu.VMEM((n_s, ROPE, rows), bf),
            pltpu.VMEM((n_d, pairs, rows, PAIR), bf),
            pltpu.VMEM((heads, seq, KDIM), bf),
            pltpu.VMEM((heads, seq, 2 * VDIM), bf),
            pltpu.VMEM((2 * rows, PAIR), bf),
            pltpu.VMEM((n_d, pairs, rows, 2 * VDIM), bf),
            pltpu.VMEM((n_d, pairs, rows, 2 * VDIM), bf),
            dma, dma,
            dma((pieces,)), dma((n_s,)), dma((pieces,)), dma((n_s,)),
            dma((pieces,)), dma((pieces,)),
            *[dma((n_d, pairs))] * 4,
        ],
        compiler_params=pltpu.CompilerParams(
            has_side_effects=True, vmem_limit_bytes=60 * 1024 * 1024
        ),
        name="latent_attention",
    )(
        queries, latent, rope_key.T, latent_gain[None, :], kv_weight, gate, out_gain[None, :],
        inner, outer,
    )


def solution(mesh):
    return jax.shard_map(
        functools.partial(per_device, mesh.shape["sp"], mesh.shape["dp"]),
        mesh=mesh,
        in_specs=(
            P(("dp", "sp"), None),
            P(("dp", "sp"), None),
            P(("dp", "sp"), None),
            P(),
            P(None, "dp"),
            P(("dp", "sp"), None),
            P(),
        ),
        out_specs=P(("dp", "sp"), None),
        check_vma=False,
    )
```
